256 devices in a mesh: grp: 2 (over y), sp: 16 (over z), tp: 8 (over x, core).
Axes of the slice: x: 4, y: 2, z: 16, core: 2. Of those that a mesh axis runs over, the one named last changes fastest.
The devices are a block of a 4x16x16 slice.
Arguments:
- stream: bfloat16 [98304, 4096], P(('grp', 'sp', 'tp')), parts along dimension 0, may hold values from -6 to 6
- norm_gain: float32 [2, 4096], replicated, may hold values from 0.1 to 1.9
- mix_weight: bfloat16 [2, 4, 1024, 1024], P(None, None, 'sp', 'tp'), may hold values from -0.1875 to 0.1875
- branch_scale: float32 [2, 4096], replicated, may hold values from 0.1 to 1.9
Outputs:
- result: bfloat16 [98304, 4096], P(('grp', 'sp', 'tp')), parts along dimension 0
The draws below stay inside these ranges and needn't reach their ends.
There are 2 independent parts, one for each index of `grp`. The reference program is written for one: setup_inputs(seed, part) draws one part's arguments, and reference() takes and returns one part's arrays. A program takes and returns all parts, laid end to end along the dimension named above; an argument that names none is the same for every part. Nothing has to cross between parts.
All inputs are finite; a program needn't handle non-finite values.
Results may differ from the reference program's by a relative error of at most 0.0056.
Values may be sent and summed in bfloat16 or wider, within the bound.
A program may use at most 128 MiB of HBM per device.

```python
import jax
import jax.numpy as jnp
from jax import lax

GW = 1024
G = 4
D = 4096
LAYERS = 2
TOKENS = 49152


def block_scale(own_key, shape, split, low, top_value):
    factor_of = 1.0
    for axis_at, blocks in split:
        steps = jax.random.uniform(jax.random.fold_in(jax.random.fold_in(own_key, 6), axis_at), (blocks,), jnp.float32, low / len(split), top_value / len(split))
        factor_of = factor_of * jnp.repeat(jnp.exp(steps), shape[axis_at] // blocks).reshape((-1,) + (1,) * (len(shape) - 1 - axis_at))
    return factor_of


def gaussian(key, shape, scale, bound, cuts=(), kind=jnp.bfloat16):
    loudness = block_scale(key, shape, cuts, -0.22, 0.18) if cuts else 1.0
    values = jax.random.normal(key, shape, jnp.float32) * scale * loudness
    return jnp.minimum(jnp.maximum(values, -bound), bound).astype(kind)


def setup_inputs(seed: int = 0, part: int = 0) -> dict:
    streams_of = jax.random.split(jax.random.key(seed), 5)
    part_splits = jax.random.split(jax.random.fold_in(streams_of[4], part), 5)
    stream = gaussian(part_splits[0], (TOKENS, D), 1.0, 6.0, ((0, 128),))
    norm_gain = jnp.clip(1.0 + 0.18 * jax.random.normal(streams_of[1], (LAYERS, D), jnp.float32), 0.1, 1.9)
    mix_weight = gaussian(streams_of[2], (LAYERS, G, GW, GW), GW ** -0.5, 0.1875, ((2, 16), (3, 8)))
    branch_scale = jnp.clip(1.0 + 0.18 * jax.random.normal(streams_of[3], (LAYERS, D), jnp.float32), 0.1, 1.9)
    return dict(stream=stream, norm_gain=norm_gain, mix_weight=mix_weight, branch_scale=branch_scale)


epsilon = 1e-06
window_lengths = (2, 4, 8, 16)

def trailing_sum(group_block, window_len):
    running = group_block
    for back_step in range(1, window_len):
        shifted = jnp.concatenate([jnp.zeros((back_step, group_block.shape[1]), jnp.float32), group_block[:-back_step]], axis=0)
        running = running + shifted
    return running

def reference(stream, norm_gain, mix_weight, branch_scale):
    residual = stream.astype(jnp.float32)
    counts_base = jnp.arange(TOKENS, dtype=jnp.float32) + 1.0
    for layer_idx in range(LAYERS):
        scale_rows = lax.rsqrt(lax.optimization_barrier(jnp.mean(residual * residual, axis=1, keepdims=True)) + epsilon)
        normed = (residual * scale_rows * norm_gain[layer_idx]).astype(jnp.bfloat16)
        outputs = []
        for group_idx in range(G):
            window_len = window_lengths[group_idx]
            group_block = normed[:, group_idx * GW:(group_idx + 1) * GW].astype(jnp.float32)
            window_mean = trailing_sum(group_block, window_len) / jnp.minimum(counts_base, float(window_len))[:, None]
            pooled = (window_mean - group_block).astype(jnp.bfloat16)
            outputs.append(jnp.dot(pooled, mix_weight[layer_idx, group_idx], preferred_element_type=jnp.float32))
        residual = residual + jnp.concatenate(outputs, axis=1) * branch_scale[layer_idx]
    return residual.astype(jnp.bfloat16)
```

```python
import functools

import jax
import jax.numpy as jnp
from jax import lax
from jax.experimental import pallas as pl
from jax.experimental.pallas import tpu as pltpu
from jax.sharding import PartitionSpec as P

MESH = pl.DeviceIdType.MESH
F32 = jnp.float32
BF16 = jnp.bfloat16

LAYERS = 2
GROUPS = 4
SLOTS = 2
HALO = 32
EPS = 1e-06
CORES = 2
RING = 16
SIDE = 4
CW, CCW = 0, 1
SPLIT = 80
BLOCK = 112
BLOCK_SKIP = 16


def kernel(stream, mixw, gain, bscale, out, W, xs, nb, pb, res, ob, own_ss, peer_ss, scale, band,
           stage_sem, peer_sem, row_sem, prow_sem, halo_sem, ss_sem, zA, zB, xF, xL, xS, bX, bS,
           s_peer, s_prow, s_halo, s_ss, s_zA, s_xA, s_zB, s_xB, out_l, out_s, out_r):
    z = lax.axis_index("sp")
    tp = lax.axis_index("tp")
    x = tp // CORES
    core = lax.rem(tp, CORES)
    peer = 1 - core
    own_rows = stream.shape[0]
    gw = stream.shape[1] // GROUPS
    depth = mixw.shape[2]
    shard = mixw.shape[3]
    wide = CORES * shard
    rows = xs.shape[0]
    chip_rows = CORES * own_rows

    def group_of(c, s):
        return c if s == 0 else GROUPS - 1 - c

    def ring_z(d):
        return lax.rem(z + (1 if d == CW else RING - 1), RING)

    def ring_x(step):
        return lax.rem(x + step + SIDE, SIDE)

    def at_z(d):
        return {"sp": ring_z(d)}

    def at_x(step):
        return {"tp": ring_x(step) * CORES + core}

    at_peer = {"tp": x * CORES + peer}

    def source_z(d, r):
        return lax.rem(z + (RING - r if d == CW else r), RING)

    def send(src, dst, ssem, rsem, dev):
        pltpu.make_async_remote_copy(
            src_ref=src, dst_ref=dst, send_sem=ssem, recv_sem=rsem, device_id=dev, device_id_type=MESH
        ).start()

    def arrived(ref, sem):
        pltpu.make_async_copy(ref, ref, sem).wait()

    chip = z * SIDE + x
    chips = RING * SIDE
    ahead = lax.rem(chip + 1, chips)
    behind = lax.rem(chip + chips - 1, chips)
    barrier = pltpu.get_barrier_semaphore()

    def greet(dev):
        pl.semaphore_signal(barrier, inc=1, device_id=dev, device_id_type=MESH)

    for dev in (at_z(CW), at_z(CCW), at_x(1), at_x(-1), at_peer,
                {"sp": behind // SIDE, "tp": lax.rem(behind, SIDE) * CORES + CORES - 1}):
        greet(dev)

    stage = []
    for l in range(LAYERS):
        for s in range(SLOTS):
            cp = pltpu.make_async_copy(
                mixw.at[l, group_of(core, s)],
                W.at[l, x, z, pl.ds(s * depth, depth), pl.ds(pl.multiple_of(core * shard, 128), shard)],
                stage_sem.at[l, s],
            )
            cp.start()
            stage.append(cp)
    local_rows = []
    for s in range(SLOTS):
        cp = pltpu.make_async_copy(
            stream.at[:, pl.ds(pl.multiple_of(group_of(core, s) * gw, 128), gw)],
            xs.at[pl.ds(pl.multiple_of(HALO + core * own_rows, 16), own_rows), pl.ds(s * gw, gw)],
            row_sem.at[s],
        )
        cp.start()
        local_rows.append(cp)

    @pl.when(core == CORES - 1)
    def _():
        pl.semaphore_wait(barrier, 7)

    @pl.when(core != CORES - 1)
    def _():
        pl.semaphore_wait(barrier, 5)

    def peer_block(l, s):
        return W.at[l, x, z, pl.ds(s * depth, depth), pl.ds(pl.multiple_of(core * shard, 128), shard)]

    for l in range(LAYERS):
        for s in range(SLOTS):
            send(mixw.at[l, group_of(peer, s)], peer_block(l, s), s_peer.at[l, s], peer_sem.at[l, s], at_peer)

    def peer_rows(s):
        return (
            stream.at[:, pl.ds(pl.multiple_of(group_of(peer, s) * gw, 128), gw)],
            xs.at[pl.ds(pl.multiple_of(HALO + core * own_rows, 16), own_rows), pl.ds(s * gw, gw)],
        )

    for s in range(SLOTS):
        src, dst = peer_rows(s)
        send(src, dst, s_prow.at[s], prow_sem.at[s], at_peer)

    def part_a(l, xx, zz):
        return W.at[l, xx, zz, pl.ds(0, SPLIT), :]

    def part_b(l, xx, zz):
        return W.at[l, xx, zz, pl.ds(SPLIT, SLOTS * depth - SPLIT), :]

    def pair_b(l, sub, zz):
        half = x // 2 if sub == 0 else 1 - x // 2
        return W.at[l, pl.ds(2 * half, 2), zz, pl.ds(SPLIT, SLOTS * depth - SPLIT), :]

    def x_sends(l, d, r, src):
        if d == CW:
            send(src, src, s_xA.at[l], xF.at[l, CW, r], at_x(1))
            send(src, src, s_xA.at[l], xL.at[l, CW], at_x(-1))
        else:
            send(src, src, s_xA.at[l], xF.at[l, CCW, r], at_x(-1))
            send(src, src, s_xA.at[l], xL.at[l, CCW], at_x(1))

    def major(l):
        return CW if l == 0 else CCW

    def on_a(l, d, r, onward):
        src = part_a(l, x, source_z(d, r))
        arrived(src, zA.at[l, d, r - 1])
        if onward:
            send(src, src, s_zA.at[l], zA.at[l, d, r], at_z(d))
        x_sends(l, d, r, src)

    def on_xf(l, d, r):
        src = part_a(l, ring_x(-1 if d == CW else 1), source_z(d, r))
        arrived(src, xF.at[l, d, r])
        send(src, src, s_xA.at[l], xS.at[l], at_x(1 if d == CW else -1))

    def on_b(l, sub, d, r, onward):
        src = pair_b(l, sub, source_z(d, r))
        arrived(src, zB.at[l, sub, d, r - 1])
        if onward:
            send(src, src, s_zB.at[l], zB.at[l, sub, d, r], at_z(d))

    def first_a(l):
        src = part_a(l, x, z)
        for d in (CW, CCW):
            send(src, src, s_zA.at[l], zA.at[l, d, 0], at_z(d))
        x_sends(l, 1 - major(l), 0, src)

    def first_bx(l):
        src = part_b(l, x, z)
        send(src, src, s_xB.at[l], bX.at[l, CW], at_x(1))
        send(src, src, s_xB.at[l], bX.at[l, CCW], at_x(-1))

    def on_bx(l):
        from_left = part_b(l, ring_x(-1), z)
        from_right = part_b(l, ring_x(1), z)
        arrived(from_left, bX.at[l, CW])
        if l == 0:
            send(from_left, from_left, s_xB.at[l], bS.at[l], at_x(1))
        arrived(from_right, bX.at[l, CCW])
        if l == 1:
            send(from_right, from_right, s_xB.at[l], bS.at[l], at_x(-1))

    def first_b(l, sub):
        src = pair_b(l, sub, z)
        for d in (CW, CCW):
            send(src, src, s_zB.at[l], zB.at[l, sub, d, 0], at_z(d))

    def on_bs(l):
        far = part_b(l, ring_x(2), z)
        arrived(far, bS.at[l])

    for l in range(LAYERS):
        for s in range(SLOTS):
            stage[l * SLOTS + s].wait()
            got = W.at[l, x, z, pl.ds(s * depth, depth), pl.ds(pl.multiple_of(peer * shard, 128), shard)]
            arrived(got, peer_sem.at[l, s])
        if l == 0:
            first_a(0)
        first_bx(l)

    def halo_pair(c, s):
        return (
            stream.at[pl.ds(own_rows - HALO, HALO), pl.ds(group_of(c, s) * gw, gw)],
            xs.at[pl.ds(0, HALO), pl.ds(s * gw, gw)],
        )

    @pl.when(core == CORES - 1)
    def _():
        for c in range(CORES):
            for s in range(SLOTS):
                src, dst = halo_pair(c, s)
                send(src, dst, s_halo.at[c, s], halo_sem.at[s],
                     {"sp": ahead // SIDE, "tp": lax.rem(ahead, SIDE) * CORES + c})

    def window(s):
        return lax.shift_left(jnp.int32(2), group_of(core, s))

    def load_rows():
        for s in range(SLOTS):
            local_rows[s].wait()
            arrived(xs.at[pl.ds(pl.multiple_of(HALO + peer * own_rows, 16), own_rows), pl.ds(s * gw, gw)],
                    prow_sem.at[s])
            arrived(xs.at[pl.ds(0, HALO), pl.ds(s * gw, gw)], halo_sem.at[s])

        @pl.when(chip == 0)
        def _():
            xs[pl.ds(0, HALO), :] = jnp.zeros((HALO, SLOTS * gw), BF16)

    def squares():
        def body(i, carry):
            at = pl.ds(pl.multiple_of(i * 32, 32), 32)
            total = None
            for k in range(SLOTS * gw // 128):
                v = xs[at, k * 128:(k + 1) * 128].astype(F32)
                total = v * v if total is None else total + v * v
            own_ss[0, at, :] = total
            return carry

        lax.fori_loop(0, rows // 32, body, 0)

    def send_ss(l):
        send(own_ss.at[l], peer_ss.at[l], s_ss.at[l], ss_sem.at[l], at_peer)

    def scales(l):
        arrived(peer_ss.at[l], ss_sem.at[l])
        total = jnp.sum(own_ss[l] + peer_ss[l], axis=1, keepdims=True)
        s = lax.rsqrt(total / float(GROUPS * gw) + EPS)
        scale[...] = jnp.broadcast_to(s, (rows, 128))

    def normalize(l):
        src = xs if l == 0 else res
        gains = [gain[l:l + 1, pl.ds(pl.multiple_of(group_of(core, s) * gw, 128), gw)] for s in range(SLOTS)]

        def body(i, carry):
            at = pl.ds(pl.multiple_of(i * 32, 32), 32)
            sc = scale[at, :]
            for s in range(SLOTS):
                for k in range(gw // 128):
                    col = slice(s * gw + k * 128, s * gw + (k + 1) * 128)
                    v = src[at, col].astype(F32)
                    nb[at, col] = (v * sc * gains[s][:, k * 128:(k + 1) * 128]).astype(BF16)
            return carry

        lax.fori_loop(0, rows // 32, body, 0)

    first_row = chip * chip_rows - HALO

    def pool(i):
        base = i * BLOCK
        above = pl.ds(pl.multiple_of(base, 16), BLOCK + BLOCK_SKIP)
        here = pl.ds(pl.multiple_of(base + BLOCK_SKIP, 16), BLOCK)
        to = pl.ds(pl.multiple_of(base, 16), BLOCK)
        count = first_row + base + BLOCK_SKIP + 1 + lax.broadcasted_iota(jnp.int32, (BLOCK, 128), 0)
        for s in range(SLOTS):
            inverse = 1.0 / jnp.maximum(jnp.minimum(count, window(s)), 1).astype(F32)
            for k in range(gw // 256):
                cols = slice(s * gw + k * 256, s * gw + (k + 1) * 256)
                total = jnp.dot(band[s], nb[above, cols], preferred_element_type=F32)
                for h in range(2):
                    col = slice(s * gw + k * 256 + h * 128, s * gw + k * 256 + (h + 1) * 128)
                    mean = total[:, h * 128:(h + 1) * 128] * inverse
                    pb[to, col] = (mean - nb[here, col].astype(F32)).astype(BF16)

    def mix(l, s, xx):
        lhs = pb[:, pl.ds(pl.multiple_of(s * gw, 128), gw)]
        w = W[l, xx, :, pl.ds(pl.multiple_of(s * depth, 16), depth), :].reshape(RING * depth, wide)
        total = jnp.dot(lhs, w, preferred_element_type=F32)
        g = jnp.where(s == 0, core, GROUPS - 1 - core)
        gcol = pl.ds(pl.multiple_of(g * gw + xx * wide, 128), wide)
        col = pl.ds(pl.multiple_of(s * gw + xx * wide, 128), wide)
        by = bscale[l:l + 1, gcol]
        if l == 0:
            r = xs[BLOCK_SKIP:, col].astype(F32) + total * by
            res[BLOCK_SKIP:, col] = r
            own_ss[1, BLOCK_SKIP:, :] += r[:, :128] * r[:, :128] + r[:, 128:] * r[:, 128:]
        else:
            r = res[HALO:, col] + total[HALO - BLOCK_SKIP:] * by
            p = s * SIDE + xx
            ob[p] = r.astype(BF16)
            mine = pl.ds(pl.multiple_of(core * own_rows, 16), own_rows)
            theirs = pl.ds(pl.multiple_of(peer * own_rows, 16), own_rows)
            send(ob.at[p, theirs], out.at[:, gcol], out_s, out_r, at_peer)
            pltpu.make_async_copy(ob.at[p, mine], out.at[:, gcol], out_l).start()

    for s in range(SLOTS):
        gap = BLOCK_SKIP + lax.broadcasted_iota(jnp.int32, (BLOCK, BLOCK + BLOCK_SKIP), 0) - lax.broadcasted_iota(
            jnp.int32, (BLOCK, BLOCK + BLOCK_SKIP), 1)
        band[s] = jnp.where((gap >= 0) & (gap < window(s)), 1.0, 0.0).astype(BF16)
    own_ss[1] = jnp.zeros((rows, 128), F32)
    res[:BLOCK_SKIP, :] = jnp.zeros((BLOCK_SKIP, SLOTS * gw), F32)

    on_bx(0)
    first_b(0, 0)
    load_rows()
    squares()
    send_ss(0)
    on_bs(0)
    first_b(0, 1)
    on_bx(1)

    last = RING // 2

    def body0(r, carry):
        on_a(0, CW, r, True)
        on_a(0, CCW, r, True)
        on_xf(0, CCW, r - 1)

        @pl.when(r > 1)
        def _():
            on_xf(0, CW, r - 1)

        @pl.when(r == 1)
        def _():
            scales(0)
            normalize(0)

        on_b(0, 0, CW, r, True)
        on_b(0, 0, CCW, r, True)
        pool(r - 1)
        on_b(0, 1, CW, r, True)
        on_b(0, 1, CCW, r, True)
        return carry

    lax.fori_loop(1, last - 1, body0, 0)
    r = last - 1
    on_a(0, CW, r, True)
    on_a(0, CCW, r, False)
    on_xf(0, CCW, r - 1)
    on_xf(0, CW, r - 1)
    on_bs(1)
    on_b(0, 0, CW, r, True)
    on_b(0, 0, CCW, r, False)
    first_a(1)
    pool(r - 1)
    on_b(0, 1, CW, r, False)
    on_b(0, 1, CCW, r, True)
    first_b(1, 0)
    first_b(1, 1)
    r = last
    on_a(0, CW, r, False)
    on_xf(0, CCW, r - 1)
    on_xf(0, CW, r - 1)
    on_b(0, 0, CW, r, False)
    on_b(0, 1, CCW, r, False)

    def finish_gather0():
        arrived(W.at[0, ring_x(1), pl.ds(0, last), pl.ds(0, SPLIT), :], xL.at[0, CW])
        arrived(W.at[0, ring_x(-1), pl.ds(0, last), pl.ds(0, SPLIT), :], xL.at[0, CCW])
        arrived(W.at[0, ring_x(2), :, pl.ds(0, SPLIT), :], xS.at[0])

    def filler(r, spot):
        q = (r - 2) * 3 + spot

        @pl.when((q >= 0) & (q < SLOTS * SIDE))
        def _():
            mix(0, q // SIDE, lax.rem(q, SIDE))

        if spot == 2:
            @pl.when(r == 4)
            def _():
                send_ss(1)

        if spot == 0:
            @pl.when(r == 5)
            def _():
                scales(1)
                normalize(1)

        i = (r - 5) * 3 + spot - 1

        @pl.when((i >= 0) & (i < rows // BLOCK))
        def _():
            pool(i)

    def body1(r, carry):
        on_a(1, CW, r, True)
        on_a(1, CCW, r, True)
        on_xf(1, CW, r - 1)

        @pl.when(r > 1)
        def _():
            on_xf(1, CCW, r - 1)

        @pl.when(r == 1)
        def _():
            on_xf(0, CW, last)

        @pl.when(r == 2)
        def _():
            finish_gather0()

        filler(r, 0)
        on_b(1, 0, CW, r, True)
        on_b(1, 0, CCW, r, True)
        filler(r, 1)
        on_b(1, 1, CW, r, True)
        on_b(1, 1, CCW, r, True)
        filler(r, 2)
        return carry

    lax.fori_loop(1, last - 1, body1, 0)
    r = last - 1
    on_a(1, CW, r, False)
    on_a(1, CCW, r, True)
    on_xf(1, CW, r - 1)
    on_xf(1, CCW, r - 1)
    on_b(1, 0, CW, r, True)
    on_b(1, 0, CCW, r, False)
    pool(5)
    on_b(1, 1, CW, r, False)
    on_b(1, 1, CCW, r, True)
    pool(6)
    r = last
    on_a(1, CCW, r, False)
    on_xf(1, CW, r - 1)
    on_xf(1, CCW, r - 1)
    on_b(1, 0, CW, r, False)
    on_b(1, 1, CCW, r, False)

    def both(xx):
        def body(s, carry):
            mix(1, s, xx)
            return carry

        lax.fori_loop(0, SLOTS, body, 0)

    def tail(j, carry):
        @pl.when(j == 1)
        def _():
            on_xf(1, CCW, last)
            arrived(W.at[1, ring_x(-1), pl.ds(0, last), pl.ds(0, SPLIT), :], xL.at[1, CCW])
            arrived(W.at[1, ring_x(1), pl.ds(0, last), pl.ds(0, SPLIT), :], xL.at[1, CW])

        @pl.when(j == 3)
        def _():
            arrived(W.at[1, ring_x(2), :, pl.ds(0, SPLIT), :], xS.at[1])

        step = jnp.where(j == 2, 3, jnp.where(j == 3, 2, j))
        both(lax.rem(x + step, SIDE))
        return carry

    lax.fori_loop(0, SIDE, tail, 0)

    for l in range(LAYERS):
        arrived(W.at[l, 0, pl.ds(0, RING - 1), pl.ds(0, SPLIT), :], s_zA.at[l])
        arrived(W.at[l, pl.ds(0, SIDE - 1), :, pl.ds(0, SPLIT), :], s_xA.at[l])
        arrived(W.at[l, pl.ds(0, SIDE - 1), 0, pl.ds(SPLIT, SLOTS * depth - SPLIT), :], s_xB.at[l])
        arrived(W.at[l, :, pl.ds(0, RING - 1), pl.ds(SPLIT, SLOTS * depth - SPLIT), :], s_zB.at[l])
        arrived(own_ss.at[l], s_ss.at[l])
        for s in range(SLOTS):
            arrived(peer_block(l, s), s_peer.at[l, s])
    for s in range(SLOTS):
        arrived(peer_rows(s)[1], s_prow.at[s])

    @pl.when(core == CORES - 1)
    def _():
        for c in range(CORES):
            for s in range(SLOTS):
                arrived(halo_pair(c, s)[1], s_halo.at[c, s])

    for sem in (out_s, out_r, out_l):
        arrived(ob.at[:, pl.ds(0, own_rows), :], sem)


def per_device(stream, norm_gain, mix_weight, branch_scale):
    own_rows, width = stream.shape
    depth, shard = mix_weight.shape[2:]
    rows = HALO + CORES * own_rows
    half = SLOTS * width // GROUPS
    wide = CORES * shard
    dma = pltpu.SemaphoreType.DMA
    last = RING // 2
    any_space = pl.BlockSpec(memory_space=pl.ANY)
    vmem = pl.BlockSpec(memory_space=pltpu.VMEM)
    return pl.pallas_call(
        kernel,
        out_shape=jax.ShapeDtypeStruct((own_rows, width), BF16),
        in_specs=[any_space, any_space, vmem, vmem],
        out_specs=any_space,
        scratch_shapes=[
            pltpu.VMEM((LAYERS, SIDE, RING, SLOTS * depth, wide), BF16),
            pltpu.VMEM((rows, half), BF16),
            pltpu.VMEM((rows, half), BF16),
            pltpu.VMEM((rows - BLOCK_SKIP, half), BF16),
            pltpu.VMEM((rows, half), F32),
            pltpu.VMEM((SLOTS * SIDE, CORES * own_rows, wide), BF16),
            pltpu.VMEM((LAYERS, rows, 128), F32),
            pltpu.VMEM((LAYERS, rows, 128), F32),
            pltpu.VMEM((rows, 128), F32),
            pltpu.VMEM((SLOTS, BLOCK, BLOCK + BLOCK_SKIP), BF16),
            dma((LAYERS, SLOTS)),
            dma((LAYERS, SLOTS)),
            dma((SLOTS,)),
            dma((SLOTS,)),
            dma((SLOTS,)),
            dma((LAYERS,)),
            dma((LAYERS, 2, last)),
            dma((LAYERS, 2, 2, last)),
            dma((LAYERS, 2, last + 1)),
            dma((LAYERS, 2)),
            dma((LAYERS,)),
            dma((LAYERS, 2)),
            dma((LAYERS,)),
            dma((LAYERS, SLOTS)),
            dma((SLOTS,)),
            dma((CORES, SLOTS)),
            dma((LAYERS,)),
            dma((LAYERS,)),
            dma((LAYERS,)),
            dma((LAYERS,)),
            dma((LAYERS,)),
            dma(()),
            dma(()),
            dma(()),
        ],
        compiler_params=pltpu.CompilerParams(
            collective_id=0, has_side_effects=True, vmem_limit_bytes=60 * 1024 * 1024
        ),
        cost_estimate=pl.CostEstimate(flops=7 * 10**9, bytes_accessed=10**7, transcendentals=0),
    )(stream, mix_weight, norm_gain, branch_scale)


def solution(mesh):
    assert mesh.shape["sp"] == RING and mesh.shape["tp"] == SIDE * CORES
    return jax.shard_map(
        per_device,
        mesh=mesh,
        in_specs=(P(("grp", "sp", "tp"), None), P(), P(None, None, "sp", "tp"), P()),
        out_specs=P(("grp", "sp", "tp"), None),
        check_vma=False,
    )
```

```python
import functools

import jax
import jax.numpy as jnp
from jax import lax
from jax.experimental import pallas as pl
from jax.experimental.pallas import tpu as pltpu
from jax.sharding import PartitionSpec as P

MESH = pl.DeviceIdType.MESH
F32 = jnp.float32
BF16 = jnp.bfloat16

LAYERS = 2
GROUPS = 4
SLOTS = 2
HALO = 32
EPS = 1e-06
CORES = 2
RING = 16
SIDE = 4
CW, CCW = 0, 1
OFFSET = 4
SPLIT = 80
BLOCK = 112
BLOCK_SKIP = 16


def kernel(stream, mixw, gain_hbm, bscale_hbm, out, gain, bscale, W, xs, wst, rst, nb, pb, res, ob, own_ss, peer_ss, scale, band,
           vec_sem, stage_sem, wst_sem, rst_sem, peer_sem, row_sem, prow_sem, halo_sem, ss_sem, zA, zB, xF, xL, xS, bX, bS,
           s_peer, s_prow, s_halo, s_ss, s_zA, s_xA, s_zB, s_xB, out_s, out_r):
    z = lax.axis_index("sp")
    tp = lax.axis_index("tp")
    x = tp // CORES
    core = lax.rem(tp, CORES)
    peer = 1 - core
    own_rows = stream.shape[0]
    gw = stream.shape[1] // GROUPS
    depth = mixw.shape[2]
    shard = mixw.shape[3]
    wide = CORES * shard
    rows = xs.shape[0]
    chip_rows = CORES * own_rows

    def group_of(c, s):
        return c if s == 0 else GROUPS - 1 - c

    def ring_z(d):
        return lax.rem(z + (1 if d == CW else RING - 1), RING)

    def ring_x(step):
        return lax.rem(x + step + SIDE, SIDE)

    def at_z(d):
        return {"sp": ring_z(d)}

    def at_x(step):
        return {"tp": ring_x(step) * CORES + core}

    at_peer = {"tp": x * CORES + peer}

    def source_z(d, r):
        return lax.rem(z + (RING - r if d == CW else r), RING)

    def send(src, dst, ssem, rsem, dev):
        pltpu.make_async_remote_copy(
            src_ref=src, dst_ref=dst, send_sem=ssem, recv_sem=rsem, device_id=dev, device_id_type=MESH
        ).start()

    def arrived(ref, sem):
        pltpu.make_async_copy(ref, ref, sem).wait()

    chip = z * SIDE + x
    chips = RING * SIDE
    ahead = lax.rem(chip + 1, chips)
    behind = lax.rem(chip + chips - 1, chips)
    barrier = pltpu.get_barrier_semaphore()

    def greet(dev):
        pl.semaphore_signal(barrier, inc=1, device_id=dev, device_id_type=MESH)

    for dev in (at_z(CW), at_z(CCW), at_x(1), at_x(-1), at_peer,
                {"sp": behind // SIDE, "tp": lax.rem(behind, SIDE) * CORES + CORES - 1}):
        greet(dev)

    stage, peer_stage = [], []
    for l in range(LAYERS):
        for s in range(SLOTS):
            cp = pltpu.make_async_copy(
                mixw.at[l, group_of(core, s)],
                W.at[l, x, z, pl.ds(s * depth, depth), pl.ds(pl.multiple_of(core * shard, 128), shard)],
                stage_sem.at[l, s],
            )
            cp.start()
            stage.append(cp)
            cp = pltpu.make_async_copy(mixw.at[l, group_of(peer, s)], wst.at[l, s], wst_sem.at[l, s])
            cp.start()
            peer_stage.append(cp)
    local_rows, peer_cols = [], []
    for s in range(SLOTS):
        cp = pltpu.make_async_copy(
            stream.at[:, pl.ds(pl.multiple_of(group_of(core, s) * gw, 128), gw)],
            xs.at[pl.ds(pl.multiple_of(HALO + core * own_rows, 16), own_rows), pl.ds(s * gw, gw)],
            row_sem.at[s],
        )
        cp.start()
        local_rows.append(cp)
        cp = pltpu.make_async_copy(
            stream.at[:, pl.ds(pl.multiple_of(group_of(peer, s) * gw, 128), gw)],
            rst.at[:, pl.ds(s * gw, gw)],
            rst_sem.at[s],
        )
        cp.start()
        peer_cols.append(cp)

    vectors = [pltpu.make_async_copy(gain_hbm, gain, vec_sem.at[0]), pltpu.make_async_copy(bscale_hbm, bscale, vec_sem.at[1])]
    for cp in vectors:
        cp.start()

    @pl.when(core == CORES - 1)
    def _():
        pl.semaphore_wait(barrier, 7)

    @pl.when(core != CORES - 1)
    def _():
        pl.semaphore_wait(barrier, 5)

    def peer_block(l, s):
        return W.at[l, x, z, pl.ds(s * depth, depth), pl.ds(pl.multiple_of(core * shard, 128), shard)]

    for l in range(LAYERS):
        for s in range(SLOTS):
            peer_stage[l * SLOTS + s].wait()
            send(wst.at[l, s], peer_block(l, s), s_peer.at[l, s], peer_sem.at[l, s], at_peer)

    def peer_rows(s):
        return (
            rst.at[:, pl.ds(s * gw, gw)],
            xs.at[pl.ds(pl.multiple_of(HALO + core * own_rows, 16), own_rows), pl.ds(s * gw, gw)],
        )

    def part_a(l, xx, zz):
        return W.at[l, xx, zz, pl.ds(0, SPLIT), :]

    def part_b(l, xx, zz):
        return W.at[l, xx, zz, pl.ds(SPLIT, SLOTS * depth - SPLIT), :]

    def pair_b(l, sub, zz):
        half = x // 2 if sub == 0 else 1 - x // 2
        return W.at[l, pl.ds(2 * half, 2), zz, pl.ds(SPLIT, SLOTS * depth - SPLIT), :]

    def x_sends(l, d, r, src):
        if d == CW:
            send(src, src, s_xA.at[l], xF.at[l, CW, r], at_x(1))
            send(src, src, s_xA.at[l], xL.at[l, CW], at_x(-1))
        else:
            send(src, src, s_xA.at[l], xF.at[l, CCW, r], at_x(-1))
            send(src, src, s_xA.at[l], xL.at[l, CCW], at_x(1))

    def major(l):
        return CW if l == 0 else CCW

    last = RING // 2

    def on_a(l, d, r):
        end = last if d == major(l) else last - 1

        @pl.when((r >= 1) & (r <= end))
        def _():
            src = part_a(l, x, source_z(d, r))
            arrived(src, zA.at[l, d, r - 1])

            @pl.when(r < end)
            def _():
                send(src, src, s_zA.at[l], zA.at[l, d, r], at_z(d))

            x_sends(l, d, r, src)

    def on_xf(l, d, r):
        first = 1 if d == major(l) else 0

        @pl.when((r >= first) & (r < first + last))
        def _():
            src = part_a(l, ring_x(-1 if d == CW else 1), source_z(d, r))
            arrived(src, xF.at[l, d, r])
            send(src, src, s_xA.at[l], xS.at[l], at_x(1 if d == CW else -1))

    def on_b(l, sub, d, r):
        end = last if d == sub else last - 1

        @pl.when((r >= 1) & (r <= end))
        def _():
            src = pair_b(l, sub, source_z(d, r))
            arrived(src, zB.at[l, sub, d, r - 1])

            @pl.when(r < end)
            def _():
                send(src, src, s_zB.at[l], zB.at[l, sub, d, r], at_z(d))

    def first_a(l):
        src = part_a(l, x, z)
        for d in (CW, CCW):
            send(src, src, s_zA.at[l], zA.at[l, d, 0], at_z(d))
        x_sends(l, 1 - major(l), 0, src)

    def first_bx(l):
        src = part_b(l, x, z)
        send(src, src, s_xB.at[l], bX.at[l, CW], at_x(1))
        send(src, src, s_xB.at[l], bX.at[l, CCW], at_x(-1))

    def on_bx(l):
        from_left = part_b(l, ring_x(-1), z)
        from_right = part_b(l, ring_x(1), z)
        arrived(from_left, bX.at[l, CW])
        if l == 0:
            send(from_left, from_left, s_xB.at[l], bS.at[l], at_x(1))
        arrived(from_right, bX.at[l, CCW])
        if l == 1:
            send(from_right, from_right, s_xB.at[l], bS.at[l], at_x(-1))

    def first_b(l, sub):
        src = pair_b(l, sub, z)
        for d in (CW, CCW):
            send(src, src, s_zB.at[l], zB.at[l, sub, d, 0], at_z(d))

    def on_bs(l):
        far = part_b(l, ring_x(2), z)
        arrived(far, bS.at[l])

    for l in range(LAYERS):
        for s in range(SLOTS):
            stage[l * SLOTS + s].wait()
            got = W.at[l, x, z, pl.ds(s * depth, depth), pl.ds(pl.multiple_of(peer * shard, 128), shard)]
            arrived(got, peer_sem.at[l, s])
        first_bx(l)
        if l == 0:
            first_a(0)

    for s in range(SLOTS):
        peer_cols[s].wait()
        src, dst = peer_rows(s)
        send(src, dst, s_prow.at[s], prow_sem.at[s], at_peer)
        local_rows[s].wait()

    def halo_pair(c, s):
        cols = pl.ds(s * gw, gw)
        src = xs.at[pl.ds(HALO + CORES * own_rows - HALO, HALO), cols] if c == CORES - 1 else rst.at[
            pl.ds(own_rows - HALO, HALO), cols]
        return src, xs.at[pl.ds(0, HALO), cols]

    @pl.when(core == CORES - 1)
    def _():
        for c in range(CORES):
            for s in range(SLOTS):
                src, dst = halo_pair(c, s)
                send(src, dst, s_halo.at[c, s], halo_sem.at[s],
                     {"sp": ahead // SIDE, "tp": lax.rem(ahead, SIDE) * CORES + c})

    def window(s):
        return lax.shift_left(jnp.int32(2), group_of(core, s))

    def load_rows():
        for cp in vectors:
            cp.wait()
        for s in range(SLOTS):
            arrived(xs.at[pl.ds(pl.multiple_of(HALO + peer * own_rows, 16), own_rows), pl.ds(s * gw, gw)],
                    prow_sem.at[s])
            arrived(xs.at[pl.ds(0, HALO), pl.ds(s * gw, gw)], halo_sem.at[s])

        @pl.when(chip == 0)
        def _():
            xs[pl.ds(0, HALO), :] = jnp.zeros((HALO, SLOTS * gw), BF16)

    def squares():
        def body(i, carry):
            at = pl.ds(pl.multiple_of(i * 32, 32), 32)
            total = None
            for k in range(SLOTS * gw // 128):
                v = xs[at, k * 128:(k + 1) * 128].astype(F32)
                total = v * v if total is None else total + v * v
            own_ss[0, at, :] = total
            return carry

        lax.fori_loop(0, rows // 32, body, 0)

    def send_ss(l):
        send(own_ss.at[l], peer_ss.at[l], s_ss.at[l], ss_sem.at[l], at_peer)

    def scales(l):
        arrived(peer_ss.at[l], ss_sem.at[l])
        total = jnp.sum(own_ss[l] + peer_ss[l], axis=1, keepdims=True)
        s = lax.rsqrt(total / float(GROUPS * gw) + EPS)
        scale[...] = jnp.broadcast_to(s, (rows, 128))

    def normalize(l):
        src = xs if l == 0 else res
        gains = [gain[l:l + 1, pl.ds(pl.multiple_of(group_of(core, s) * gw, 128), gw)] for s in range(SLOTS)]

        def body(i, carry):
            at = pl.ds(pl.multiple_of(i * 32, 32), 32)
            sc = scale[at, :]
            for s in range(SLOTS):
                for k in range(gw // 128):
                    col = slice(s * gw + k * 128, s * gw + (k + 1) * 128)
                    v = src[at, col].astype(F32)
                    nb[at, col] = (v * sc * gains[s][:, k * 128:(k + 1) * 128]).astype(BF16)
            return carry

        lax.fori_loop(0, rows // 32, body, 0)

    first_row = chip * chip_rows - HALO

    def pool(i):
        base = i * BLOCK
        above = pl.ds(pl.multiple_of(base, 16), BLOCK + BLOCK_SKIP)
        here = pl.ds(pl.multiple_of(base + BLOCK_SKIP, 16), BLOCK)
        to = pl.ds(pl.multiple_of(base, 16), BLOCK)
        count = first_row + base + BLOCK_SKIP + 1 + lax.broadcasted_iota(jnp.int32, (BLOCK, 128), 0)
        for s in range(SLOTS):
            inverse = 1.0 / jnp.maximum(jnp.minimum(count, window(s)), 1).astype(F32)
            for k in range(gw // 256):
                cols = slice(s * gw + k * 256, s * gw + (k + 1) * 256)
                total = jnp.dot(band[s], nb[above, cols], preferred_element_type=F32)
                for h in range(2):
                    col = slice(s * gw + k * 256 + h * 128, s * gw + k * 256 + (h + 1) * 128)
                    mean = total[:, h * 128:(h + 1) * 128] * inverse
                    pb[to, col] = (mean - nb[here, col].astype(F32)).astype(BF16)

    def mix(l, s, xx):
        lhs = pb[:, pl.ds(pl.multiple_of(s * gw, 128), gw)]
        w = W[l, xx, :, pl.ds(pl.multiple_of(s * depth, 16), depth), :].reshape(RING * depth, wide)
        total = jnp.dot(lhs, w, preferred_element_type=F32)
        g = jnp.where(s == 0, core, GROUPS - 1 - core)
        gcol = pl.ds(pl.multiple_of(g * gw + xx * wide, 128), wide)
        col = pl.ds(pl.multiple_of(s * gw + xx * wide, 128), wide)
        by = bscale[l:l + 1, gcol]
        if l == 0:
            r = xs[BLOCK_SKIP:, col].astype(F32) + total * by
            res[BLOCK_SKIP:, col] = r
            own_ss[1, BLOCK_SKIP:, :] += r[:, :128] * r[:, :128] + r[:, 128:] * r[:, 128:]
        else:
            r = res[HALO:, col] + total[HALO - BLOCK_SKIP:] * by
            p = s * SIDE + xx

            def share(mine, theirs):
                out[:, gcol] = r[mine].astype(BF16)
                ob[p] = r[theirs].astype(BF16)

            @pl.when(core == 0)
            def _():
                share(slice(0, own_rows), slice(own_rows, None))

            @pl.when(core != 0)
            def _():
                share(slice(own_rows, None), slice(0, own_rows))

            send(ob.at[p], out.at[:, gcol], out_s, out_r, at_peer)

    for s in range(SLOTS):
        gap = BLOCK_SKIP + lax.broadcasted_iota(jnp.int32, (BLOCK, BLOCK + BLOCK_SKIP), 0) - lax.broadcasted_iota(
            jnp.int32, (BLOCK, BLOCK + BLOCK_SKIP), 1)
        band[s] = jnp.where((gap >= 0) & (gap < window(s)), 1.0, 0.0).astype(BF16)
    own_ss[1] = jnp.zeros((rows, 128), F32)
    res[:BLOCK_SKIP, :] = jnp.zeros((BLOCK_SKIP, SLOTS * gw), F32)

    def finish_gather(l, hop):
        if hop == 1:
            arrived(W.at[l, ring_x(1), pl.ds(0, last), pl.ds(0, SPLIT), :], xL.at[l, CW])
            arrived(W.at[l, ring_x(-1), pl.ds(0, last), pl.ds(0, SPLIT), :], xL.at[l, CCW])
        else:
            arrived(W.at[l, ring_x(2), :, pl.ds(0, SPLIT), :], xS.at[l])

    def mix_many(l, start, stop):
        def body(q, carry):
            k = q // SLOTS
            flip = jnp.where(k == 2, 3, jnp.where(k == 3, 2, k))
            mix(l, lax.rem(q, SLOTS), lax.bitwise_xor(x, flip))
            return carry

        lax.fori_loop(start, stop, body, 0)

    def pool_many(start, stop):
        def body(i, carry):
            pool(i)
            return carry

        lax.fori_loop(start, stop, body, 0)

    full = 2 + last

    def filler(g, spot):
        if spot == 0:
            @pl.when(g == 2)
            def _():
                load_rows()
                squares()
                send_ss(0)

            @pl.when(g == 3)
            def _():
                scales(0)
                normalize(0)

        if spot == 2:
            @pl.when(g == full + 1)
            def _():
                scales(1)
                normalize(1)

        e = (g - full - 2) * 3 + spot
        start = 2 * jnp.where(g <= full, (g - 4) if spot == 1 else -1, e)
        start = jnp.where(start < 0, rows // BLOCK, start)
        pool_many(start, jnp.minimum(start + 2, rows // BLOCK))

        for l in range(LAYERS):
            done = full + l * OFFSET
            if spot == 2:
                @pl.when(g == done - 1)
                def _(l=l):
                    mix_many(l, 0, SLOTS)

                @pl.when(g == done)
                def _(l=l):
                    mix_many(l, 2 * SLOTS, 3 * SLOTS)
                    finish_gather(l, 2)
                    mix_many(l, 3 * SLOTS, 4 * SLOTS)
                    if l == 0:
                        send_ss(1)

            if spot == 0:
                @pl.when(g == done)
                def _(l=l):
                    finish_gather(l, 1)
                    mix_many(l, SLOTS, 2 * SLOTS)

    def step(g, carry):
        for l in range(LAYERS):
            for d in (CW, CCW):
                on_a(l, d, g - l * OFFSET)

        @pl.when(g == OFFSET)
        def _():
            first_a(1)

        @pl.when(g == 1)
        def _():
            on_bx(0)
            first_b(0, 0)

        filler(g, 0)
        for l in range(LAYERS):
            for d in (CW, CCW):
                on_b(l, 0, d, g - l * OFFSET - 1)
        for l in range(LAYERS):
            for d in (CW, CCW):
                on_xf(l, d, g - l * OFFSET - 1)

        @pl.when(g == 2)
        def _():
            on_bs(0)
            first_b(0, 1)

        @pl.when(g == 3)
        def _():
            on_bx(1)

        @pl.when(g == OFFSET + 1)
        def _():
            first_b(1, 0)

        filler(g, 1)
        for l in range(LAYERS):
            for d in (CW, CCW):
                on_b(l, 1, d, g - l * OFFSET - 2)

        @pl.when(g == OFFSET + 2)
        def _():
            on_bs(1)
            first_b(1, 1)

        filler(g, 2)
        return carry

    lax.fori_loop(1, OFFSET + full + 1, step, 0)

    for l in range(LAYERS):
        arrived(W.at[l, 0, pl.ds(0, RING - 1), pl.ds(0, SPLIT), :], s_zA.at[l])
        arrived(W.at[l, pl.ds(0, SIDE - 1), :, pl.ds(0, SPLIT), :], s_xA.at[l])
        arrived(W.at[l, pl.ds(0, SIDE - 1), 0, pl.ds(SPLIT, SLOTS * depth - SPLIT), :], s_xB.at[l])
        arrived(W.at[l, :, pl.ds(0, RING - 1), pl.ds(SPLIT, SLOTS * depth - SPLIT), :], s_zB.at[l])
        arrived(own_ss.at[l], s_ss.at[l])
        for s in range(SLOTS):
            arrived(peer_block(l, s), s_peer.at[l, s])
    for s in range(SLOTS):
        arrived(peer_rows(s)[1], s_prow.at[s])

    @pl.when(core == CORES - 1)
    def _():
        for c in range(CORES):
            for s in range(SLOTS):
                arrived(halo_pair(c, s)[1], s_halo.at[c, s])

    for sem in (out_s, out_r):
        arrived(ob, sem)


def per_device(stream, norm_gain, mix_weight, branch_scale):
    own_rows, width = stream.shape
    depth, shard = mix_weight.shape[2:]
    rows = HALO + CORES * own_rows
    half = SLOTS * width // GROUPS
    wide = CORES * shard
    dma = pltpu.SemaphoreType.DMA
    last = RING // 2
    hbm = pl.BlockSpec(memory_space=pltpu.HBM)
    vmem = pl.BlockSpec(memory_space=pltpu.VMEM)
    return pl.pallas_call(
        kernel,
        out_shape=jax.ShapeDtypeStruct((own_rows, width), BF16),
        in_specs=[hbm] * 4,
        out_specs=vmem,
        scratch_shapes=[
            pltpu.VMEM(norm_gain.shape, F32),
            pltpu.VMEM(branch_scale.shape, F32),
            pltpu.VMEM((LAYERS, SIDE, RING, SLOTS * depth, wide), BF16),
            pltpu.VMEM((rows, half), BF16),
            pltpu.VMEM((LAYERS, SLOTS, depth, shard), BF16),
            pltpu.VMEM((own_rows, half), BF16),
            pltpu.VMEM((rows, half), BF16),
            pltpu.VMEM((rows - BLOCK_SKIP, half), BF16),
            pltpu.VMEM((rows, half), F32),
            pltpu.VMEM((SLOTS * SIDE, own_rows, wide), BF16),
            pltpu.VMEM((LAYERS, rows, 128), F32),
            pltpu.VMEM((LAYERS, rows, 128), F32),
            pltpu.VMEM((rows, 128), F32),
            pltpu.VMEM((SLOTS, BLOCK, BLOCK + BLOCK_SKIP), BF16),
            dma((2,)),
            dma((LAYERS, SLOTS)),
            dma((LAYERS, SLOTS)),
            dma((SLOTS,)),
            dma((LAYERS, SLOTS)),
            dma((SLOTS,)),
            dma((SLOTS,)),
            dma((SLOTS,)),
            dma((LAYERS,)),
            dma((LAYERS, 2, last)),
            dma((LAYERS, 2, 2, last)),
            dma((LAYERS, 2, last + 1)),
            dma((LAYERS, 2)),
            dma((LAYERS,)),
            dma((LAYERS, 2)),
            dma((LAYERS,)),
            dma((LAYERS, SLOTS)),
            dma((SLOTS,)),
            dma((CORES, SLOTS)),
            dma((LAYERS,)),
            dma((LAYERS,)),
            dma((LAYERS,)),
            dma((LAYERS,)),
            dma((LAYERS,)),
            dma(()),
            dma(()),
        ],
        compiler_params=pltpu.CompilerParams(
            collective_id=0, has_side_effects=True, vmem_limit_bytes=40 * 1024 * 1024
        ),
        cost_estimate=pl.CostEstimate(flops=7 * 10**9, bytes_accessed=10**7, transcendentals=0),
    )(*(pltpu.with_memory_space_constraint(v, pltpu.HBM) for v in (stream, mix_weight, norm_gain, branch_scale)))


def solution(mesh):
    assert mesh.shape["sp"] == RING and mesh.shape["tp"] == SIDE * CORES
    return jax.shard_map(
        per_device,
        mesh=mesh,
        in_specs=(P(("grp", "sp", "tp"), None), P(), P(None, None, "sp", "tp"), P()),
        out_specs=P(("grp", "sp", "tp"), None),
        check_vma=False,
    )
```

```python
import functools

import jax
import jax.numpy as jnp
from jax import lax
from jax.experimental import pallas as pl
from jax.experimental.pallas import tpu as pltpu
from jax.sharding import PartitionSpec as P

MESH = pl.DeviceIdType.MESH
F32 = jnp.float32
BF16 = jnp.bfloat16

LAYERS = 2
GROUPS = 4
SLOTS = 2
HALO = 32
EPS = 1e-06
CORES = 2
RING = 16
SIDE = 4
CW, CCW = 0, 1
START_A = (0, 2)
START_B = ((0, 1, 1, 2), (2, 5, 5, 6))
FLIP = (0, 1, 3, 2)
PIECES = ((0, 80),)
SPLIT = 80
BLOCK = 112
BLOCK_SKIP = 16


def kernel(stream, mixw, gain_hbm, bscale_hbm, out, gain, bscale, W, xs, wst, rst, nb, pb, res, ob, own_ss, peer_ss, scale, band,
           vec_sem, stage_sem, wst_sem, rst_sem, peer_sem, row_sem, prow_sem, halo_sem, ss_sem, zA, zB, xF, xL, xS, bX, bS,
           s_peer, s_prow, s_halo, s_ss, s_zA, s_xA, s_zB, s_xB, out_s, out_r):
    z = lax.axis_index("sp")
    tp = lax.axis_index("tp")
    x = tp // CORES
    core = lax.rem(tp, CORES)
    peer = 1 - core
    own_rows = stream.shape[0]
    gw = stream.shape[1] // GROUPS
    depth = mixw.shape[2]
    shard = mixw.shape[3]
    wide = CORES * shard
    rows = xs.shape[0]
    chip_rows = CORES * own_rows

    def group_of(c, s):
        return c if s == 0 else GROUPS - 1 - c

    def ring_z(d):
        return lax.rem(z + (1 if d == CW else RING - 1), RING)

    def ring_x(step):
        return lax.rem(x + step + SIDE, SIDE)

    def at_z(d):
        return {"sp": ring_z(d)}

    def at_x(step):
        return {"tp": ring_x(step) * CORES + core}

    at_peer = {"tp": x * CORES + peer}

    def source_z(d, r):
        return lax.rem(z + (RING - r if d == CW else r), RING)

    def send(src, dst, ssem, rsem, dev):
        pltpu.make_async_remote_copy(
            src_ref=src, dst_ref=dst, send_sem=ssem, recv_sem=rsem, device_id=dev, device_id_type=MESH
        ).start()

    def arrived(ref, sem):
        pltpu.make_async_copy(ref, ref, sem).wait()

    chip = z * SIDE + x
    chips = RING * SIDE
    ahead = lax.rem(chip + 1, chips)
    behind = lax.rem(chip + chips - 1, chips)
    barrier = pltpu.get_barrier_semaphore()

    def greet(dev):
        pl.semaphore_signal(barrier, inc=1, device_id=dev, device_id_type=MESH)

    for dev in (at_z(CW), at_z(CCW), at_x(1), at_x(-1), at_peer,
                {"sp": behind // SIDE, "tp": lax.rem(behind, SIDE) * CORES + CORES - 1}):
        greet(dev)

    stage, peer_stage = [], []
    for l in range(LAYERS):
        for s in range(SLOTS):
            cp = pltpu.make_async_copy(
                mixw.at[l, group_of(core, s)],
                W.at[l, x, z, pl.ds(s * depth, depth), pl.ds(pl.multiple_of(core * shard, 128), shard)],
                stage_sem.at[l, s],
            )
            cp.start()
            stage.append(cp)
            cp = pltpu.make_async_copy(mixw.at[l, group_of(peer, s)], wst.at[l, s], wst_sem.at[l, s])
            cp.start()
            peer_stage.append(cp)
    local_rows, peer_cols = [], []
    for s in range(SLOTS):
        cp = pltpu.make_async_copy(
            stream.at[:, pl.ds(pl.multiple_of(group_of(core, s) * gw, 128), gw)],
            xs.at[pl.ds(pl.multiple_of(HALO + core * own_rows, 16), own_rows), pl.ds(s * gw, gw)],
            row_sem.at[s],
        )
        cp.start()
        local_rows.append(cp)
        cp = pltpu.make_async_copy(
            stream.at[:, pl.ds(pl.multiple_of(group_of(peer, s) * gw, 128), gw)],
            rst.at[:, pl.ds(s * gw, gw)],
            rst_sem.at[s],
        )
        cp.start()
        peer_cols.append(cp)

    vectors = [pltpu.make_async_copy(gain_hbm, gain, vec_sem.at[0]), pltpu.make_async_copy(bscale_hbm, bscale, vec_sem.at[1])]
    for cp in vectors:
        cp.start()

    @pl.when(core == CORES - 1)
    def _():
        pl.semaphore_wait(barrier, 7)

    @pl.when(core != CORES - 1)
    def _():
        pl.semaphore_wait(barrier, 5)

    def peer_block(l, s):
        return W.at[l, x, z, pl.ds(s * depth, depth), pl.ds(pl.multiple_of(core * shard, 128), shard)]

    for l in range(LAYERS):
        for s in range(SLOTS):
            peer_stage[l * SLOTS + s].wait()
            send(wst.at[l, s], peer_block(l, s), s_peer.at[l, s], peer_sem.at[l, s], at_peer)

    def peer_rows(s):
        return (
            rst.at[:, pl.ds(s * gw, gw)],
            xs.at[pl.ds(pl.multiple_of(HALO + core * own_rows, 16), own_rows), pl.ds(s * gw, gw)],
        )

    def part_a(l, xx, zz):
        return W.at[l, xx, zz, pl.ds(0, SPLIT), :]

    def part_b(l, xx, zz):
        return W.at[l, xx, zz, pl.ds(SPLIT, SLOTS * depth - SPLIT), :]

    def slab_b(l, k, zz):
        return part_b(l, lax.bitwise_xor(x, FLIP[k]), zz)

    def piece_a(l, p, zz):
        return W.at[l, x, zz, pl.ds(*PIECES[p]), :]

    def x_sends(l, d, r, src):
        if d == CW:
            send(src, src, s_xA.at[l], xF.at[l, CW, r], at_x(1))
            send(src, src, s_xA.at[l], xL.at[l, CW], at_x(-1))
        else:
            send(src, src, s_xA.at[l], xF.at[l, CCW, r], at_x(-1))
            send(src, src, s_xA.at[l], xL.at[l, CCW], at_x(1))

    def major(l):
        return CW if l == 0 else CCW

    last = RING // 2

    def on_a(l, d, r):
        end = last if d == major(l) else last - 1

        @pl.when((r >= 1) & (r <= end))
        def _():
            zz = source_z(d, r)
            for p in range(len(PIECES)):
                src = piece_a(l, p, zz)
                arrived(src, zA.at[l, p, d, r - 1])

                @pl.when(r < end)
                def _():
                    send(src, src, s_zA.at[l], zA.at[l, p, d, r], at_z(d))

            x_sends(l, d, r, part_a(l, x, zz))

    def on_xf(l, d, r):
        first = 1 if d == major(l) else 0

        @pl.when((r >= first) & (r < first + last))
        def _():
            src = part_a(l, ring_x(-1 if d == CW else 1), source_z(d, r))
            arrived(src, xF.at[l, d, r])
            send(src, src, s_xA.at[l], xS.at[l], at_x(1 if d == CW else -1))

    def on_b(l, k, d, r):
        end = last if d == k % 2 else last - 1

        @pl.when((r >= 1) & (r <= end))
        def _():
            src = slab_b(l, k, source_z(d, r))
            arrived(src, zB.at[l, k, d, r - 1])

            @pl.when(r < end)
            def _():
                send(src, src, s_zB.at[l], zB.at[l, k, d, r], at_z(d))

    def first_a(l):
        src = part_a(l, x, z)
        for p in range(len(PIECES)):
            for d in (CW, CCW):
                piece = piece_a(l, p, z)
                send(piece, piece, s_zA.at[l], zA.at[l, p, d, 0], at_z(d))
        x_sends(l, 1 - major(l), 0, src)

    def first_bx(l):
        src = part_b(l, x, z)
        send(src, src, s_xB.at[l], bX.at[l, CW], at_x(1))
        send(src, src, s_xB.at[l], bX.at[l, CCW], at_x(-1))

    def on_bx(l):
        from_left = part_b(l, ring_x(-1), z)
        from_right = part_b(l, ring_x(1), z)
        arrived(from_right, bX.at[l, CCW])
        if l == 0:
            send(from_right, from_right, s_xB.at[l], bS.at[l], at_x(-1))
        arrived(from_left, bX.at[l, CW])
        if l == 1:
            send(from_left, from_left, s_xB.at[l], bS.at[l], at_x(1))

    def first_b(l, k):
        src = slab_b(l, k, z)
        for d in (CW, CCW):
            send(src, src, s_zB.at[l], zB.at[l, k, d, 0], at_z(d))

    def on_bs(l):
        far = part_b(l, ring_x(2), z)
        arrived(far, bS.at[l])

    for l in range(LAYERS):
        for s in range(SLOTS):
            stage[l * SLOTS + s].wait()
            got = W.at[l, x, z, pl.ds(s * depth, depth), pl.ds(pl.multiple_of(peer * shard, 128), shard)]
            arrived(got, peer_sem.at[l, s])
        first_bx(l)
        if l == 0:
            first_a(0)
            first_b(0, 0)

    for s in range(SLOTS):
        peer_cols[s].wait()
        src, dst = peer_rows(s)
        send(src, dst, s_prow.at[s], prow_sem.at[s], at_peer)
        local_rows[s].wait()

    def halo_pair(c, s):
        cols = pl.ds(s * gw, gw)
        src = xs.at[pl.ds(HALO + CORES * own_rows - HALO, HALO), cols] if c == CORES - 1 else rst.at[
            pl.ds(own_rows - HALO, HALO), cols]
        return src, xs.at[pl.ds(0, HALO), cols]

    @pl.when(core == CORES - 1)
    def _():
        for c in range(CORES):
            for s in range(SLOTS):
                src, dst = halo_pair(c, s)
                send(src, dst, s_halo.at[c, s], halo_sem.at[s],
                     {"sp": ahead // SIDE, "tp": lax.rem(ahead, SIDE) * CORES + c})

    def window(s):
        return lax.shift_left(jnp.int32(2), group_of(core, s))

    def load_rows():
        for cp in vectors:
            cp.wait()
        for s in range(SLOTS):
            arrived(xs.at[pl.ds(pl.multiple_of(HALO + peer * own_rows, 16), own_rows), pl.ds(s * gw, gw)],
                    prow_sem.at[s])
            arrived(xs.at[pl.ds(0, HALO), pl.ds(s * gw, gw)], halo_sem.at[s])

        @pl.when(chip == 0)
        def _():
            xs[pl.ds(0, HALO), :] = jnp.zeros((HALO, SLOTS * gw), BF16)

    def squares():
        def body(i, carry):
            at = pl.ds(pl.multiple_of(i * 32, 32), 32)
            total = None
            for k in range(SLOTS * gw // 128):
                v = xs[at, k * 128:(k + 1) * 128].astype(F32)
                total = v * v if total is None else total + v * v
            own_ss[0, at, :] = total
            return carry

        lax.fori_loop(0, rows // 32, body, 0)

    def send_ss(l):
        send(own_ss.at[l], peer_ss.at[l], s_ss.at[l], ss_sem.at[l], at_peer)

    def scales(l):
        arrived(peer_ss.at[l], ss_sem.at[l])
        total = jnp.sum(own_ss[l] + peer_ss[l], axis=1, keepdims=True)
        s = lax.rsqrt(total / float(GROUPS * gw) + EPS)
        scale[...] = jnp.broadcast_to(s, (rows, 128))

    def normalize(l):
        src = xs if l == 0 else res
        gains = [gain[l:l + 1, pl.ds(pl.multiple_of(group_of(core, s) * gw, 128), gw)] for s in range(SLOTS)]

        def body(i, carry):
            at = pl.ds(pl.multiple_of(i * 32, 32), 32)
            sc = scale[at, :]
            for s in range(SLOTS):
                for k in range(gw // 128):
                    col = slice(s * gw + k * 128, s * gw + (k + 1) * 128)
                    v = src[at, col].astype(F32)
                    nb[at, col] = (v * sc * gains[s][:, k * 128:(k + 1) * 128]).astype(BF16)
            return carry

        lax.fori_loop(0, rows // 32, body, 0)

    first_row = chip * chip_rows - HALO

    def pool(i):
        base = i * BLOCK
        above = pl.ds(pl.multiple_of(base, 16), BLOCK + BLOCK_SKIP)
        here = pl.ds(pl.multiple_of(base + BLOCK_SKIP, 16), BLOCK)
        to = pl.ds(pl.multiple_of(base, 16), BLOCK)
        count = first_row + base + BLOCK_SKIP + 1 + lax.broadcasted_iota(jnp.int32, (BLOCK, 128), 0)
        for s in range(SLOTS):
            inverse = 1.0 / jnp.maximum(jnp.minimum(count, window(s)), 1).astype(F32)
            for k in range(gw // 256):
                cols = slice(s * gw + k * 256, s * gw + (k + 1) * 256)
                total = jnp.dot(band[s], nb[above, cols], preferred_element_type=F32)
                for h in range(2):
                    col = slice(s * gw + k * 256 + h * 128, s * gw + k * 256 + (h + 1) * 128)
                    mean = total[:, h * 128:(h + 1) * 128] * inverse
                    pb[to, col] = (mean - nb[here, col].astype(F32)).astype(BF16)

    def mix(l, s, xx):
        lhs = pb[:, pl.ds(pl.multiple_of(s * gw, 128), gw)]
        w = W[l, xx, :, pl.ds(pl.multiple_of(s * depth, 16), depth), :].reshape(RING * depth, wide)
        total = jnp.dot(lhs, w, preferred_element_type=F32)
        g = jnp.where(s == 0, core, GROUPS - 1 - core)
        gcol = pl.ds(pl.multiple_of(g * gw + xx * wide, 128), wide)
        col = pl.ds(pl.multiple_of(s * gw + xx * wide, 128), wide)
        by = bscale[l:l + 1, gcol]
        if l == 0:
            r = xs[BLOCK_SKIP:, col].astype(F32) + total * by
            res[BLOCK_SKIP:, col] = r
            own_ss[1, BLOCK_SKIP:, :] += r[:, :128] * r[:, :128] + r[:, 128:] * r[:, 128:]
        else:
            r = res[HALO:, col] + total[HALO - BLOCK_SKIP:] * by
            p = s * SIDE + xx

            def share(mine, theirs):
                out[:, gcol] = r[mine].astype(BF16)
                ob[p] = r[theirs].astype(BF16)

            @pl.when(core == 0)
            def _():
                share(slice(0, own_rows), slice(own_rows, None))

            @pl.when(core != 0)
            def _():
                share(slice(own_rows, None), slice(0, own_rows))

            send(ob.at[p], out.at[:, gcol], out_s, out_r, at_peer)

    for s in range(SLOTS):
        gap = BLOCK_SKIP + lax.broadcasted_iota(jnp.int32, (BLOCK, BLOCK + BLOCK_SKIP), 0) - lax.broadcasted_iota(
            jnp.int32, (BLOCK, BLOCK + BLOCK_SKIP), 1)
        band[s] = jnp.where((gap >= 0) & (gap < window(s)), 1.0, 0.0).astype(BF16)
    own_ss[1] = jnp.zeros((rows, 128), F32)
    res[:BLOCK_SKIP, :] = jnp.zeros((BLOCK_SKIP, SLOTS * gw), F32)

    def finish_gather(l, hop):
        if hop == 1:
            arrived(W.at[l, ring_x(1), pl.ds(0, last), pl.ds(0, SPLIT), :], xL.at[l, CW])
            arrived(W.at[l, ring_x(-1), pl.ds(0, last), pl.ds(0, SPLIT), :], xL.at[l, CCW])
        else:
            arrived(W.at[l, ring_x(2), :, pl.ds(0, SPLIT), :], xS.at[l])

    def mix_many(l, start, stop):
        def body(q, carry):
            k = q // SLOTS
            flip = jnp.where(k == 2, 3, jnp.where(k == 3, 2, k))
            mix(l, lax.rem(q, SLOTS), lax.bitwise_xor(x, flip))
            return carry

        lax.fori_loop(start, stop, body, 0)

    def pool_many(start, stop):
        def body(i, carry):
            pool(i)
            return carry

        lax.fori_loop(start, stop, body, 0)

    full, full1 = (max(START_A[l] + 2, *START_B[l]) + last for l in range(LAYERS))

    def filler(g, spot):
        if spot == 0:
            @pl.when(g == 2)
            def _():
                load_rows()
                squares()
                send_ss(0)

            @pl.when(g == 3)
            def _():
                scales(0)
                normalize(0)

        if spot == 2:
            @pl.when(g == full + 1)
            def _():
                scales(1)
                normalize(1)

        e = (g - full - 2) * 3 + spot
        start = 2 * jnp.where(g <= full, (g - 4) if spot == 1 else -1, e)
        start = jnp.where(start < 0, rows // BLOCK, start)
        pool_many(start, jnp.minimum(start + 2, rows // BLOCK))

        for l, at, where, k, slabs, hop in (
            (0, full - 2, 2, 0, 1, 0), (0, full - 1, 2, 1, 1, 1), (0, full, 0, 2, 1, 0), (0, full, 2, 3, 1, 2),
            (1, full1 - 1, 1, 0, 1, 0), (1, full1 - 1, 2, 1, 1, 1), (1, full1, 0, 2, 1, 0), (1, full1, 2, 3, 1, 2),
        ):
            if where == spot:
                @pl.when(g == at)
                def _(l=l, k=k, slabs=slabs, hop=hop):
                    if hop:
                        finish_gather(l, hop)
                    mix_many(l, SLOTS * k, SLOTS * (k + slabs))
                    if l == 0 and hop == 2:
                        send_ss(1)

    def step(g, carry):
        for l in range(LAYERS):
            for d in (CW, CCW):
                on_a(l, d, g - START_A[l])

        @pl.when(g == START_A[1])
        def _():
            first_a(1)

        def begin(l, *lanes):
            for k in lanes:
                @pl.when(g == START_B[l][k])
                def _(k=k):
                    first_b(l, k)

        @pl.when(g == START_B[0][1])
        def _():
            on_bx(0)

        begin(0, 1, 2)

        @pl.when(g == START_B[0][3])
        def _():
            on_bs(0)

        begin(1, 0)
        filler(g, 0)
        for k in (0, 1):
            for l in range(LAYERS):
                for d in (CW, CCW):
                    on_b(l, k, d, g - START_B[l][k])
        for l in range(LAYERS):
            for d in (CW, CCW):
                on_xf(l, d, g - START_A[l] - 1)
        begin(0, 3)
        begin(1, 1, 2)
        filler(g, 1)
        for k in (2, 3):
            for l in range(LAYERS):
                for d in (CW, CCW):
                    on_b(l, k, d, g - START_B[l][k])

        @pl.when(g == 3)
        def _():
            on_bx(1)

        @pl.when(g == 5)
        def _():
            on_bs(1)

        begin(1, 3)
        filler(g, 2)
        return carry

    lax.fori_loop(1, full1 + 1, step, 0)

    for l in range(LAYERS):
        arrived(W.at[l, 0, pl.ds(0, RING - 1), pl.ds(0, SPLIT), :], s_zA.at[l])
        arrived(W.at[l, pl.ds(0, SIDE - 1), :, pl.ds(0, SPLIT), :], s_xA.at[l])
        arrived(W.at[l, pl.ds(0, SIDE - 1), 0, pl.ds(SPLIT, SLOTS * depth - SPLIT), :], s_xB.at[l])
        arrived(W.at[l, :, pl.ds(0, RING - 1), pl.ds(SPLIT, SLOTS * depth - SPLIT), :], s_zB.at[l])
        arrived(own_ss.at[l], s_ss.at[l])
        for s in range(SLOTS):
            arrived(peer_block(l, s), s_peer.at[l, s])
    for s in range(SLOTS):
        arrived(peer_rows(s)[1], s_prow.at[s])

    @pl.when(core == CORES - 1)
    def _():
        for c in range(CORES):
            for s in range(SLOTS):
                arrived(halo_pair(c, s)[1], s_halo.at[c, s])

    for sem in (out_s, out_r):
        arrived(ob, sem)


def per_device(stream, norm_gain, mix_weight, branch_scale):
    own_rows, width = stream.shape
    depth, shard = mix_weight.shape[2:]
    rows = HALO + CORES * own_rows
    half = SLOTS * width // GROUPS
    wide = CORES * shard
    dma = pltpu.SemaphoreType.DMA
    last = RING // 2
    hbm = pl.BlockSpec(memory_space=pltpu.HBM)
    vmem = pl.BlockSpec(memory_space=pltpu.VMEM)
    return pl.pallas_call(
        kernel,
        out_shape=jax.ShapeDtypeStruct((own_rows, width), BF16),
        in_specs=[hbm] * 4,
        out_specs=vmem,
        scratch_shapes=[
            pltpu.VMEM(norm_gain.shape, F32),
            pltpu.VMEM(branch_scale.shape, F32),
            pltpu.VMEM((LAYERS, SIDE, RING, SLOTS * depth, wide), BF16),
            pltpu.VMEM((rows, half), BF16),
            pltpu.VMEM((LAYERS, SLOTS, depth, shard), BF16),
            pltpu.VMEM((own_rows, half), BF16),
            pltpu.VMEM((rows, half), BF16),
            pltpu.VMEM((rows - BLOCK_SKIP, half), BF16),
            pltpu.VMEM((rows, half), F32),
            pltpu.VMEM((SLOTS * SIDE, own_rows, wide), BF16),
            pltpu.VMEM((LAYERS, rows, 128), F32),
            pltpu.VMEM((LAYERS, rows, 128), F32),
            pltpu.VMEM((rows, 128), F32),
            pltpu.VMEM((SLOTS, BLOCK, BLOCK + BLOCK_SKIP), BF16),
            dma((2,)),
            dma((LAYERS, SLOTS)),
            dma((LAYERS, SLOTS)),
            dma((SLOTS,)),
            dma((LAYERS, SLOTS)),
            dma((SLOTS,)),
            dma((SLOTS,)),
            dma((SLOTS,)),
            dma((LAYERS,)),
            dma((LAYERS, len(PIECES), 2, last)),
            dma((LAYERS, SIDE, 2, last)),
            dma((LAYERS, 2, last + 1)),
            dma((LAYERS, 2)),
            dma((LAYERS,)),
            dma((LAYERS, 2)),
            dma((LAYERS,)),
            dma((LAYERS, SLOTS)),
            dma((SLOTS,)),
            dma((CORES, SLOTS)),
            dma((LAYERS,)),
            dma((LAYERS,)),
            dma((LAYERS,)),
            dma((LAYERS,)),
            dma((LAYERS,)),
            dma(()),
            dma(()),
        ],
        compiler_params=pltpu.CompilerParams(
            collective_id=0, has_side_effects=True, vmem_limit_bytes=40 * 1024 * 1024
        ),
        cost_estimate=pl.CostEstimate(flops=7 * 10**9, bytes_accessed=10**7, transcendentals=0),
    )(*(pltpu.with_memory_space_constraint(v, pltpu.HBM) for v in (stream, mix_weight, norm_gain, branch_scale)))


def solution(mesh):
    assert mesh.shape["sp"] == RING and mesh.shape["tp"] == SIDE * CORES
    return jax.shard_map(
        per_device,
        mesh=mesh,
        in_specs=(P(("grp", "sp", "tp"), None), P(), P(None, None, "sp", "tp"), P()),
        out_specs=P(("grp", "sp", "tp"), None),
        check_vma=False,
    )
```

```python
import functools

import jax
import jax.numpy as jnp
from jax import lax
from jax.experimental import pallas as pl
from jax.experimental.pallas import tpu as pltpu
from jax.sharding import PartitionSpec as P

MESH = pl.DeviceIdType.MESH
F32 = jnp.float32
BF16 = jnp.bfloat16

LAYERS = 2
GROUPS = 4
SLOTS = 2
HALO = 32
EPS = 1e-06
CORES = 2
RING = 16
SIDE = 4
CW, CCW = 0, 1
START_A = (0, 2)
START_B = ((0, 1, 1, 2), (2, 5, 5, 6))
FLIP = (0, 1, 3, 2)
PIECES = ((0, 80),)
SPLIT = 80
BLOCK = 112
BLOCK_SKIP = 16


def kernel(stream, mixw, gain_hbm, bscale_hbm, out, gain, bscale, W, xs, wst, rst, nb, pb, res, ob, own_ss, peer_ss, scale, band,
           vec_sem, stage_sem, wst_sem, rst_sem, peer_sem, row_sem, prow_sem, halo_sem, ss_sem, zA, zB, xF, xL, xS, bX, bS,
           s_peer, s_prow, s_halo, s_ss, s_zA, s_xA, s_zB, s_xB, out_s, out_r):
    z = lax.axis_index("sp")
    tp = lax.axis_index("tp")
    x = tp // CORES
    core = lax.rem(tp, CORES)
    peer = 1 - core
    own_rows = stream.shape[0]
    gw = stream.shape[1] // GROUPS
    depth = mixw.shape[2]
    shard = mixw.shape[3]
    wide = CORES * shard
    rows = xs.shape[0]
    chip_rows = CORES * own_rows

    def group_of(c, s):
        return c if s == 0 else GROUPS - 1 - c

    def ring_z(d):
        return lax.rem(z + (1 if d == CW else RING - 1), RING)

    def ring_x(step):
        return lax.rem(x + step + SIDE, SIDE)

    def at_z(d):
        return {"sp": ring_z(d)}

    def at_x(step):
        return {"tp": ring_x(step) * CORES + core}

    at_peer = {"tp": x * CORES + peer}

    def source_z(d, r):
        return lax.rem(z + (RING - r if d == CW else r), RING)

    def send(src, dst, ssem, rsem, dev):
        pltpu.make_async_remote_copy(
            src_ref=src, dst_ref=dst, send_sem=ssem, recv_sem=rsem, device_id=dev, device_id_type=MESH
        ).start()

    def arrived(ref, sem):
        pltpu.make_async_copy(ref, ref, sem).wait()

    chip = z * SIDE + x
    chips = RING * SIDE
    ahead = lax.rem(chip + 1, chips)
    behind = lax.rem(chip + chips - 1, chips)
    barrier = pltpu.get_barrier_semaphore()

    def greet(dev):
        pl.semaphore_signal(barrier, inc=1, device_id=dev, device_id_type=MESH)

    for dev in (at_z(CW), at_z(CCW), at_x(1), at_x(-1), at_peer,
                {"sp": behind // SIDE, "tp": lax.rem(behind, SIDE) * CORES + CORES - 1}):
        greet(dev)

    stage, peer_stage = [], []
    for l in range(LAYERS):
        for s in range(SLOTS):
            cp = pltpu.make_async_copy(
                mixw.at[l, group_of(core, s)],
                W.at[l, x, z, pl.ds(s * depth, depth), pl.ds(pl.multiple_of(core * shard, 128), shard)],
                stage_sem.at[l, s],
            )
            cp.start()
            stage.append(cp)
            cp = pltpu.make_async_copy(mixw.at[l, group_of(peer, s)], wst.at[l, s], wst_sem.at[l, s])
            cp.start()
            peer_stage.append(cp)
    local_rows, peer_cols = [], []
    for s in range(SLOTS):
        cp = pltpu.make_async_copy(
            stream.at[:, pl.ds(pl.multiple_of(group_of(core, s) * gw, 128), gw)],
            xs.at[pl.ds(pl.multiple_of(HALO + core * own_rows, 16), own_rows), pl.ds(s * gw, gw)],
            row_sem.at[s],
        )
        cp.start()
        local_rows.append(cp)
        cp = pltpu.make_async_copy(
            stream.at[:, pl.ds(pl.multiple_of(group_of(peer, s) * gw, 128), gw)],
            rst.at[:, pl.ds(s * gw, gw)],
            rst_sem.at[s],
        )
        cp.start()
        peer_cols.append(cp)

    vectors = [pltpu.make_async_copy(gain_hbm, gain, vec_sem.at[0]), pltpu.make_async_copy(bscale_hbm, bscale, vec_sem.at[1])]
    for cp in vectors:
        cp.start()

    @pl.when(core == CORES - 1)
    def _():
        pl.semaphore_wait(barrier, 7)

    @pl.when(core != CORES - 1)
    def _():
        pl.semaphore_wait(barrier, 5)

    def peer_block(l, s):
        return W.at[l, x, z, pl.ds(s * depth, depth), pl.ds(pl.multiple_of(core * shard, 128), shard)]

    for l in range(LAYERS):
        for s in range(SLOTS):
            peer_stage[l * SLOTS + s].wait()
            send(wst.at[l, s], peer_block(l, s), s_peer.at[l, s], peer_sem.at[l, s], at_peer)

    def peer_rows(s):
        return (
            rst.at[:, pl.ds(s * gw, gw)],
            xs.at[pl.ds(pl.multiple_of(HALO + core * own_rows, 16), own_rows), pl.ds(s * gw, gw)],
        )

    def part_a(l, xx, zz):
        return W.at[l, xx, zz, pl.ds(0, SPLIT), :]

    def part_b(l, xx, zz):
        return W.at[l, xx, zz, pl.ds(SPLIT, SLOTS * depth - SPLIT), :]

    def slab_b(l, k, zz):
        return part_b(l, lax.bitwise_xor(x, FLIP[k]), zz)

    def piece_a(l, p, zz):
        return W.at[l, x, zz, pl.ds(*PIECES[p]), :]

    def x_sends(l, d, r, src):
        if d == CW:
            send(src, src, s_xA.at[l], xF.at[l, CW, r], at_x(1))
            send(src, src, s_xA.at[l], xL.at[l, CW], at_x(-1))
        else:
            send(src, src, s_xA.at[l], xF.at[l, CCW, r], at_x(-1))
            send(src, src, s_xA.at[l], xL.at[l, CCW], at_x(1))

    def major(l):
        return CW if l == 0 else CCW

    last = RING // 2

    def on_a(l, d, r):
        end = last if d == major(l) else last - 1

        @pl.when((r >= 1) & (r <= end))
        def _():
            zz = source_z(d, r)
            for p in range(len(PIECES)):
                src = piece_a(l, p, zz)
                arrived(src, zA.at[l, p, d, r - 1])

                @pl.when(r < end)
                def _():
                    send(src, src, s_zA.at[l], zA.at[l, p, d, r], at_z(d))

            x_sends(l, d, r, part_a(l, x, zz))

    def on_xf(l, d, r):
        first = 1 if d == major(l) else 0

        @pl.when((r >= first) & (r < first + last))
        def _():
            src = part_a(l, ring_x(-1 if d == CW else 1), source_z(d, r))
            arrived(src, xF.at[l, d, r])
            send(src, src, s_xA.at[l], xS.at[l], at_x(1 if d == CW else -1))

    def on_b(l, k, d, r):
        end = last if d == k % 2 else last - 1

        @pl.when((r >= 1) & (r <= end))
        def _():
            src = slab_b(l, k, source_z(d, r))
            arrived(src, zB.at[l, k, d, r - 1])

            @pl.when(r < end)
            def _():
                send(src, src, s_zB.at[l], zB.at[l, k, d, r], at_z(d))

    def first_a(l):
        src = part_a(l, x, z)
        for p in range(len(PIECES)):
            for d in (CW, CCW):
                piece = piece_a(l, p, z)
                send(piece, piece, s_zA.at[l], zA.at[l, p, d, 0], at_z(d))
        x_sends(l, 1 - major(l), 0, src)

    def first_bx(l):
        src = part_b(l, x, z)
        send(src, src, s_xB.at[l], bX.at[l, CW], at_x(1))
        send(src, src, s_xB.at[l], bX.at[l, CCW], at_x(-1))

    def on_bx(l):
        from_left = part_b(l, ring_x(-1), z)
        from_right = part_b(l, ring_x(1), z)
        arrived(from_right, bX.at[l, CCW])
        if l == 0:
            send(from_right, from_right, s_xB.at[l], bS.at[l], at_x(-1))
        arrived(from_left, bX.at[l, CW])
        if l == 1:
            send(from_left, from_left, s_xB.at[l], bS.at[l], at_x(1))

    def first_b(l, k):
        src = slab_b(l, k, z)
        for d in (CW, CCW):
            send(src, src, s_zB.at[l], zB.at[l, k, d, 0], at_z(d))

    def on_bs(l):
        far = part_b(l, ring_x(2), z)
        arrived(far, bS.at[l])

    for l in range(LAYERS):
        for s in range(SLOTS):
            stage[l * SLOTS + s].wait()
            got = W.at[l, x, z, pl.ds(s * depth, depth), pl.ds(pl.multiple_of(peer * shard, 128), shard)]
            arrived(got, peer_sem.at[l, s])
        first_bx(l)
        if l == 0:
            first_a(0)
            first_b(0, 0)

    for s in range(SLOTS):
        peer_cols[s].wait()
        src, dst = peer_rows(s)
        send(src, dst, s_prow.at[s], prow_sem.at[s], at_peer)
        local_rows[s].wait()

    def halo_pair(c, s):
        cols = pl.ds(s * gw, gw)
        src = xs.at[pl.ds(HALO + CORES * own_rows - HALO, HALO), cols] if c == CORES - 1 else rst.at[
            pl.ds(own_rows - HALO, HALO), cols]
        return src, xs.at[pl.ds(0, HALO), cols]

    @pl.when(core == CORES - 1)
    def _():
        for c in range(CORES):
            for s in range(SLOTS):
                src, dst = halo_pair(c, s)
                send(src, dst, s_halo.at[c, s], halo_sem.at[s],
                     {"sp": ahead // SIDE, "tp": lax.rem(ahead, SIDE) * CORES + c})

    def window(s):
        return lax.shift_left(jnp.int32(2), group_of(core, s))

    def load_rows():
        for cp in vectors:
            cp.wait()
        for s in range(SLOTS):
            arrived(xs.at[pl.ds(pl.multiple_of(HALO + peer * own_rows, 16), own_rows), pl.ds(s * gw, gw)],
                    prow_sem.at[s])
            arrived(xs.at[pl.ds(0, HALO), pl.ds(s * gw, gw)], halo_sem.at[s])

        @pl.when(chip == 0)
        def _():
            xs[pl.ds(0, HALO), :] = jnp.zeros((HALO, SLOTS * gw), BF16)

    def squares():
        def body(i, carry):
            at = pl.ds(pl.multiple_of(i * 32, 32), 32)
            total = None
            for k in range(SLOTS * gw // 128):
                v = xs[at, k * 128:(k + 1) * 128].astype(F32)
                total = v * v if total is None else total + v * v
            own_ss[0, at, :] = total
            return carry

        lax.fori_loop(0, rows // 32, body, 0)

    def send_ss(l):
        send(own_ss.at[l], peer_ss.at[l], s_ss.at[l], ss_sem.at[l], at_peer)

    def scales(l):
        arrived(peer_ss.at[l], ss_sem.at[l])
        total = jnp.sum(own_ss[l] + peer_ss[l], axis=1, keepdims=True)
        s = lax.rsqrt(total / float(GROUPS * gw) + EPS)
        scale[...] = jnp.broadcast_to(s, (rows, 128))

    def normalize(l):
        src = xs if l == 0 else res
        gains = [gain[l:l + 1, pl.ds(pl.multiple_of(group_of(core, s) * gw, 128), gw)] for s in range(SLOTS)]

        def body(i, carry):
            at = pl.ds(pl.multiple_of(i * 32, 32), 32)
            sc = scale[at, :]
            for s in range(SLOTS):
                for k in range(gw // 128):
                    col = slice(s * gw + k * 128, s * gw + (k + 1) * 128)
                    v = src[at, col].astype(F32)
                    nb[at, col] = (v * sc * gains[s][:, k * 128:(k + 1) * 128]).astype(BF16)
            return carry

        lax.fori_loop(0, rows // 32, body, 0)

    first_row = chip * chip_rows - HALO

    def pool(i):
        base = i * BLOCK
        above = pl.ds(pl.multiple_of(base, 16), BLOCK + BLOCK_SKIP)
        here = pl.ds(pl.multiple_of(base + BLOCK_SKIP, 16), BLOCK)
        to = pl.ds(pl.multiple_of(base, 16), BLOCK)
        count = first_row + base + BLOCK_SKIP + 1 + lax.broadcasted_iota(jnp.int32, (BLOCK, 128), 0)
        for s in range(SLOTS):
            inverse = 1.0 / jnp.maximum(jnp.minimum(count, window(s)), 1).astype(F32)
            for k in range(gw // 256):
                cols = slice(s * gw + k * 256, s * gw + (k + 1) * 256)
                total = jnp.dot(band[s], nb[above, cols], preferred_element_type=F32)
                for h in range(2):
                    col = slice(s * gw + k * 256 + h * 128, s * gw + k * 256 + (h + 1) * 128)
                    mean = total[:, h * 128:(h + 1) * 128] * inverse
                    pb[to, col] = (mean - nb[here, col].astype(F32)).astype(BF16)

    def mix(l, s, xx):
        lhs = pb[:, pl.ds(pl.multiple_of(s * gw, 128), gw)]
        w = W[l, xx, :, pl.ds(pl.multiple_of(s * depth, 16), depth), :].reshape(RING * depth, wide)
        total = jnp.dot(lhs, w, preferred_element_type=F32)
        g = jnp.where(s == 0, core, GROUPS - 1 - core)
        gcol = pl.ds(pl.multiple_of(g * gw + xx * wide, 128), wide)
        col = pl.ds(pl.multiple_of(s * gw + xx * wide, 128), wide)
        by = bscale[l:l + 1, gcol]
        if l == 0:
            r = xs[BLOCK_SKIP:, col].astype(F32) + total * by
            res[BLOCK_SKIP:, col] = r
            own_ss[1, BLOCK_SKIP:, :] += r[:, :128] * r[:, :128] + r[:, 128:] * r[:, 128:]
        else:
            r = res[HALO:, col] + total[HALO - BLOCK_SKIP:] * by
            p = s * SIDE + xx

            def share(mine, theirs):
                out[:, gcol] = r[mine].astype(BF16)
                ob[p] = r[theirs].astype(BF16)

            @pl.when(core == 0)
            def _():
                share(slice(0, own_rows), slice(own_rows, None))

            @pl.when(core != 0)
            def _():
                share(slice(own_rows, None), slice(0, own_rows))

            send(ob.at[p], out.at[:, gcol], out_s, out_r, at_peer)

    for s in range(SLOTS):
        gap = BLOCK_SKIP + lax.broadcasted_iota(jnp.int32, (BLOCK, BLOCK + BLOCK_SKIP), 0) - lax.broadcasted_iota(
            jnp.int32, (BLOCK, BLOCK + BLOCK_SKIP), 1)
        band[s] = jnp.where((gap >= 0) & (gap < window(s)), 1.0, 0.0).astype(BF16)
    own_ss[1] = jnp.zeros((rows, 128), F32)
    res[:BLOCK_SKIP, :] = jnp.zeros((BLOCK_SKIP, SLOTS * gw), F32)

    def finish_gather(l, hop):
        if hop == 1:
            arrived(W.at[l, ring_x(1), pl.ds(0, last), pl.ds(0, SPLIT), :], xL.at[l, CW])
            arrived(W.at[l, ring_x(-1), pl.ds(0, last), pl.ds(0, SPLIT), :], xL.at[l, CCW])
        else:
            arrived(W.at[l, ring_x(2), :, pl.ds(0, SPLIT), :], xS.at[l])

    def mix_many(l, start, stop):
        def body(q, carry):
            k = q // SLOTS
            flip = jnp.where(k == 2, 3, jnp.where(k == 3, 2, k))
            mix(l, lax.rem(q, SLOTS), lax.bitwise_xor(x, flip))
            return carry

        lax.fori_loop(start, stop, body, 0)

    def pool_many(start, stop):
        def body(i, carry):
            pool(i)
            return carry

        lax.fori_loop(start, stop, body, 0)

    full, full1 = (max(START_A[l] + 2, *START_B[l]) + last for l in range(LAYERS))

    def filler(g, spot):
        if spot == 0:
            @pl.when(g == 2)
            def _():
                load_rows()
                squares()
                send_ss(0)

            @pl.when(g == 3)
            def _():
                scales(0)
                normalize(0)

        if spot == 2:
            @pl.when(g == full + 1)
            def _():
                scales(1)
                normalize(1)

        e = (g - full - 2) * 3 + spot
        start = 2 * jnp.where(g <= full, (g - 4) if spot == 1 else -1, e)
        start = jnp.where(start < 0, rows // BLOCK, start)
        pool_many(start, jnp.minimum(start + 2, rows // BLOCK))

        for l, at, where, k, slabs, hop in (
            (0, full - 2, 2, 0, 1, 0), (0, full - 1, 2, 1, 1, 1), (0, full, 0, 2, 1, 0), (0, full, 2, 3, 1, 2),
            (1, full1 - 1, 1, 0, 1, 0), (1, full1 - 1, 2, 1, 1, 1), (1, full1, 0, 2, 1, 0), (1, full1, 2, 3, 1, 2),
        ):
            if where == spot:
                @pl.when(g == at)
                def _(l=l, k=k, slabs=slabs, hop=hop):
                    if hop:
                        finish_gather(l, hop)
                    mix_many(l, SLOTS * k, SLOTS * (k + slabs))
                    if l == 0 and hop == 2:
                        send_ss(1)

    def step(g, carry):
        for l in range(LAYERS):
            for d in (CW, CCW):
                on_a(l, d, g - START_A[l])

        @pl.when(g == START_A[1])
        def _():
            first_a(1)

        def begin(l, *lanes):
            for k in lanes:
                @pl.when(g == START_B[l][k])
                def _(k=k):
                    first_b(l, k)

        @pl.when(g == START_B[0][1])
        def _():
            on_bx(0)

        begin(0, 1, 2)

        @pl.when(g == START_B[0][3])
        def _():
            on_bs(0)

        begin(1, 0)
        filler(g, 0)
        for l in range(LAYERS):
            for k in (0, 1):
                for d in (CW, CCW):
                    on_b(l, k, d, g - START_B[l][k])
        for l in range(LAYERS):
            for d in (CW, CCW):
                on_xf(l, d, g - START_A[l] - 1)
        begin(0, 3)
        begin(1, 1, 2)
        filler(g, 1)
        for l in range(LAYERS):
            for k in (2, 3):
                for d in (CW, CCW):
                    on_b(l, k, d, g - START_B[l][k])

        @pl.when(g == 3)
        def _():
            on_bx(1)

        @pl.when(g == 5)
        def _():
            on_bs(1)

        begin(1, 3)
        filler(g, 2)
        return carry

    lax.fori_loop(1, full1 + 1, step, 0)

    for l in range(LAYERS):
        arrived(W.at[l, 0, pl.ds(0, RING - 1), pl.ds(0, SPLIT), :], s_zA.at[l])
        arrived(W.at[l, pl.ds(0, SIDE - 1), :, pl.ds(0, SPLIT), :], s_xA.at[l])
        arrived(W.at[l, pl.ds(0, SIDE - 1), 0, pl.ds(SPLIT, SLOTS * depth - SPLIT), :], s_xB.at[l])
        arrived(W.at[l, :, pl.ds(0, RING - 1), pl.ds(SPLIT, SLOTS * depth - SPLIT), :], s_zB.at[l])
        arrived(own_ss.at[l], s_ss.at[l])
        for s in range(SLOTS):
            arrived(peer_block(l, s), s_peer.at[l, s])
    for s in range(SLOTS):
        arrived(peer_rows(s)[1], s_prow.at[s])

    @pl.when(core == CORES - 1)
    def _():
        for c in range(CORES):
            for s in range(SLOTS):
                arrived(halo_pair(c, s)[1], s_halo.at[c, s])

    for sem in (out_s, out_r):
        arrived(ob, sem)


def per_device(stream, norm_gain, mix_weight, branch_scale):
    own_rows, width = stream.shape
    depth, shard = mix_weight.shape[2:]
    rows = HALO + CORES * own_rows
    half = SLOTS * width // GROUPS
    wide = CORES * shard
    dma = pltpu.SemaphoreType.DMA
    last = RING // 2
    hbm = pl.BlockSpec(memory_space=pltpu.HBM)
    vmem = pl.BlockSpec(memory_space=pltpu.VMEM)
    return pl.pallas_call(
        kernel,
        out_shape=jax.ShapeDtypeStruct((own_rows, width), BF16),
        in_specs=[hbm] * 4,
        out_specs=vmem,
        scratch_shapes=[
            pltpu.VMEM(norm_gain.shape, F32),
            pltpu.VMEM(branch_scale.shape, F32),
            pltpu.VMEM((LAYERS, SIDE, RING, SLOTS * depth, wide), BF16),
            pltpu.VMEM((rows, half), BF16),
            pltpu.VMEM((LAYERS, SLOTS, depth, shard), BF16),
            pltpu.VMEM((own_rows, half), BF16),
            pltpu.VMEM((rows, half), BF16),
            pltpu.VMEM((rows - BLOCK_SKIP, half), BF16),
            pltpu.VMEM((rows, half), F32),
            pltpu.VMEM((SLOTS * SIDE, own_rows, wide), BF16),
            pltpu.VMEM((LAYERS, rows, 128), F32),
            pltpu.VMEM((LAYERS, rows, 128), F32),
            pltpu.VMEM((rows, 128), F32),
            pltpu.VMEM((SLOTS, BLOCK, BLOCK + BLOCK_SKIP), BF16),
            dma((2,)),
            dma((LAYERS, SLOTS)),
            dma((LAYERS, SLOTS)),
            dma((SLOTS,)),
            dma((LAYERS, SLOTS)),
            dma((SLOTS,)),
            dma((SLOTS,)),
            dma((SLOTS,)),
            dma((LAYERS,)),
            dma((LAYERS, len(PIECES), 2, last)),
            dma((LAYERS, SIDE, 2, last)),
            dma((LAYERS, 2, last + 1)),
            dma((LAYERS, 2)),
            dma((LAYERS,)),
            dma((LAYERS, 2)),
            dma((LAYERS,)),
            dma((LAYERS, SLOTS)),
            dma((SLOTS,)),
            dma((CORES, SLOTS)),
            dma((LAYERS,)),
            dma((LAYERS,)),
            dma((LAYERS,)),
            dma((LAYERS,)),
            dma((LAYERS,)),
            dma(()),
            dma(()),
        ],
        compiler_params=pltpu.CompilerParams(
            collective_id=0, has_side_effects=True, vmem_limit_bytes=40 * 1024 * 1024
        ),
        cost_estimate=pl.CostEstimate(flops=7 * 10**9, bytes_accessed=10**7, transcendentals=0),
    )(*(pltpu.with_memory_space_constraint(v, pltpu.HBM) for v in (stream, mix_weight, norm_gain, branch_scale)))


def solution(mesh):
    assert mesh.shape["sp"] == RING and mesh.shape["tp"] == SIDE * CORES
    return jax.shard_map(
        per_device,
        mesh=mesh,
        in_specs=(P(("grp", "sp", "tp"), None), P(), P(None, None, "sp", "tp"), P()),
        out_specs=P(("grp", "sp", "tp"), None),
        check_vma=False,
    )
```
